32 devices in a mesh: fs: 8 (over z, y), tp: 4 (over x, core).
Axes of the slice: x: 2, y: 2, z: 4, core: 2. Of those that a mesh axis runs over, the one named last changes fastest.
Arguments:
- weights_in: float32 [2, 2048, 5632], P(None, 'fs', 'tp'), may hold values from -6 to 6
- weights_mix: float32 [2048, 2048], P('fs', 'tp'), may hold values from -6 to 6
- momentum_in: float32 [2, 2048, 5632], P(None, 'fs', 'tp'), may hold values from -5 to 5
- momentum_mix: float32 [2048, 2048], P('fs', 'tp'), may hold values from -5 to 5
- grads_in: float32 [2, 2048, 5632], P(None, 'fs', 'tp'), may hold values from -5 to 5
- grads_mix: float32 [2048, 2048], P('fs', 'tp'), may hold values from -5 to 5
Outputs:
- momentum_in_next: float32 [2, 2048, 5632], P(None, 'fs', 'tp')
- momentum_mix_next: float32 [2048, 2048], P('fs', 'tp')
- weights_in_next: float32 [2, 2048, 5632], P(None, 'fs', 'tp')
- weights_mix_next: float32 [2048, 2048], P('fs', 'tp')
- update_in: float32 [2, 2048, 5632], P(None, 'fs', 'tp')
- update_mix: float32 [2048, 2048], P('fs', 'tp')
The draws below stay inside these ranges and needn't reach their ends.
All inputs are finite; a program needn't handle non-finite values.
Results may differ from the reference program's by a relative error of at most 0.0003.
Values sent between devices are 32-bit elements; how exact they have to be, the bound alone decides.
A program may use at most 128 MiB of HBM per device.

```python
import math
import jax
import jax.numpy as jnp
from jax import lax

D = 2048
FF = 5632
ITERS = 3


def unit_field(key, shape):
    return jnp.clip(jax.random.normal(key, shape, jnp.float32), -5.0, 5.0)


def draw_momentum_in(key, part):
    return unit_field(jax.random.fold_in(key, 11), (2, D, FF))


def draw_momentum_mix(key, part):
    return unit_field(jax.random.fold_in(key, 12), (D, D))


def draw_grads_in(key, part):
    return unit_field(jax.random.fold_in(key, 13), (2, D, FF))


def draw_grads_mix(key, part):
    return unit_field(jax.random.fold_in(key, 14), (D, D))


def steps_of(key, dims, cuts, smallest, top_value):
    def one(position, parts):
        draws = jax.random.uniform(jax.random.fold_in(jax.random.fold_in(key, 6), position), (parts,), jnp.float32, smallest / len(cuts), top_value / len(cuts))
        return jnp.repeat(jnp.exp(draws), dims[position] // parts).reshape((-1,) + (1,) * (len(dims) - position - 1))

    gain = one(*cuts[0])
    for cut in cuts[1:]:
        gain = gain * one(*cut)
    return gain


def noise(rng, extent, deviation, limit, cuts=(), dtype=jnp.bfloat16):
    factor_of = steps_of(rng, extent, cuts, -0.22, 0.18) if cuts else 1.0
    values = jax.random.normal(rng, extent, jnp.float32) * deviation * factor_of
    return jnp.minimum(jnp.maximum(values, -limit), limit).astype(dtype)


def setup_inputs(seed: int = 0) -> dict:
    streams_of = jax.random.split(jax.random.key(seed), 7)
    weights_in = noise(streams_of[0], (2, D, FF), 1.0, 6.0, ((1, 8), (2, 4)), jnp.float32)
    weights_mix = noise(streams_of[1], (D, D), 1.0, 6.0, ((0, 8), (1, 4)), jnp.float32)
    momentum_in = draw_momentum_in(jax.random.fold_in(streams_of[6], 71), 0)
    momentum_mix = draw_momentum_mix(jax.random.fold_in(streams_of[6], 71), 0)
    grads_in = draw_grads_in(jax.random.fold_in(streams_of[6], 71), 0)
    grads_mix = draw_grads_mix(jax.random.fold_in(streams_of[6], 71), 0)
    return {"weights_in": weights_in, "weights_mix": weights_mix, "momentum_in": momentum_in, "momentum_mix": momentum_mix, "grads_in": grads_in, "grads_mix": grads_mix}


A_COEF = 3.4445
B_COEF = -4.775
C_COEF = 2.0315
MOMENTUM_DECAY = 0.95
STEP_RATE = 0.02
HIGH = lax.Precision.HIGHEST

def orthogonal(moment):
    row_total, col_total = moment.shape
    current = moment
    for iteration in range(ITERS):
        gram_sum = jnp.dot(current, current.T, precision=HIGH)
        if iteration == 0:
            scaling = 0.5 * lax.rsqrt(jnp.maximum(jnp.trace(gram_sum) / D, 1.0))
        else:
            scaling = jnp.float32(1.0)
        square = jnp.dot(gram_sum, gram_sum, precision=HIGH)
        poly_mat = scaling ** 2 * B_COEF * gram_sum + scaling ** 4 * C_COEF * square
        current = scaling * (A_COEF * current + jnp.dot(poly_mat, current, precision=HIGH))
    return current * math.sqrt(max(row_total, col_total))

def reference(weights_in, weights_mix, momentum_in, momentum_mix, grads_in, grads_mix):
    moment_in = MOMENTUM_DECAY * momentum_in + grads_in
    moment_mix = MOMENTUM_DECAY * momentum_mix + grads_mix
    step_in = jnp.stack([orthogonal(moment_in[0]), orthogonal(moment_in[1])])
    step_mix = orthogonal(moment_mix)
    return (moment_in, moment_mix, weights_in - STEP_RATE * step_in, weights_mix - STEP_RATE * step_mix, step_in, step_mix)
```

```python
import jax
import jax.numpy as jnp
from jax import lax
from jax.experimental import pallas as pl
from jax.experimental.pallas import tpu as pltpu
from jax.sharding import Mesh, PartitionSpec as P

A_COEF = 3.4445
B_COEF = -4.775
C_COEF = 2.0315
MOMENTUM_DECAY = 0.95
STEP_RATE = 0.02
GROUPS = 4
MIX_GROUP = 0
IN_GROUPS = (1, 2)


def halves(a):
    high = lax.reduce_precision(a, exponent_bits=8, mantissa_bits=7)
    return high.astype(jnp.bfloat16), (a - high).astype(jnp.bfloat16)


def deep(a, b, dims):
    ah, al = halves(a)
    bh, bl = halves(b)
    left = jnp.concatenate([ah, al, ah], axis=dims[0])
    right = jnp.concatenate([bh, bh, bl], axis=dims[1])
    return lax.dot_general(
        left, right, (((dims[0],), (dims[1],)), ((), ())), preferred_element_type=jnp.float32
    )


def unfold(window):
    size, _, block = window.shape
    half = size // 2

    def tile(r, c):
        ahead = (r - c) % size
        if ahead <= half:
            return window[c, ahead * block : (ahead + 1) * block]
        back = size - ahead
        return window[r, back * block : (back + 1) * block].T

    return jnp.concatenate(
        [jnp.concatenate([tile(r, c) for c in range(size)], axis=1) for r in range(size)], axis=0
    )


def split_store(high_ref, low_ref, index, value):
    high = value.astype(jnp.bfloat16)
    high_ref[index] = high
    low_ref[index] = (value - high.astype(jnp.float32)).astype(jnp.bfloat16)


def thin_store(parts, index, value):
    for part in parts:
        piece = value.astype(jnp.bfloat16)
        part[index] = piece
        value = value - piece.astype(jnp.float32)


def load_gram(window_ref, scale, high_ref, low_ref):
    size, _, block = window_ref.shape
    half = size // 2

    def body(c, carry):
        at_c = pl.ds(pl.multiple_of(c * block, block), block)
        for ahead in range(half + 1):
            at_r = pl.ds(pl.multiple_of(lax.rem(c + ahead, size) * block, block), block)
            tile = window_ref[c, ahead * block : (ahead + 1) * block, :]
            if scale is not None:
                tile = tile * scale
            split_store(high_ref, low_ref, (at_r, at_c), tile)
            if 0 < ahead < half:
                split_store(high_ref, low_ref, (at_c, at_r), tile.T)
        return carry

    lax.fori_loop(0, size, body, 0)


def product(gram, pair, emit, rows_per=512, fine=False):
    high_ref, low_ref = gram
    rows_per = min(rows_per, high_ref.shape[0])

    def body(i, carry):
        rows = pl.ds(pl.multiple_of(i * rows_per, rows_per), rows_per)
        high = high_ref[rows, :]
        value = jnp.dot(high, pair[0][...], preferred_element_type=jnp.float32)
        value += jnp.dot(high, pair[1][...], preferred_element_type=jnp.float32)
        low = low_ref[rows, :]
        rest = jnp.dot(low, pair[0][...], preferred_element_type=jnp.float32)
        if fine:
            rest += jnp.dot(low, pair[1][...], preferred_element_type=jnp.float32)
            rest += jnp.dot(high, pair[2][...], preferred_element_type=jnp.float32)
        value += rest
        emit(rows, value)
        return carry

    lax.fori_loop(0, high_ref.shape[0] // rows_per, body, 0)


def poly_step(gram, v, s, pair, other, fine=False):
    def first(rows, value):
        s[rows, :] = value
        thin_store(other, (rows, slice(None)), value)

    def second(rows, value):
        value = A_COEF * v[rows, :] + B_COEF * s[rows, :] + C_COEF * value
        v[rows, :] = value
        thin_store(pair, (rows, slice(None)), value)

    product(gram, pair, first, fine=fine)
    product(gram, other, second, fine=fine)


def begin(window_ref, scale, position, v, pair):
    size, _, block = window_ref.shape
    for ahead in range(size):
        at = lax.rem(position + ahead, size)
        rows = pl.ds(pl.multiple_of(at * block, block), block)
        if ahead <= size // 2:
            value = window_ref[position, ahead * block : (ahead + 1) * block, :]
        else:
            back = size - ahead
            value = window_ref[at, back * block : (back + 1) * block, :].T
        if scale is not None:
            value = value * scale
        v[rows, :] = value
        thin_store(pair, (rows, slice(None)), value)


def next_gram_steps(gram, v, s, pair, other):
    poly_step(gram, v, s, pair, other, True)
    poly_step(gram, v, s, pair, other, True)


def put_window(v, position, out_ref, size, block):
    for ahead in range(size // 2 + 1):
        row = lax.rem(position + ahead, size) * block
        out_ref[ahead * block : (ahead + 1) * block, :] = v[
            pl.ds(pl.multiple_of(row, block), block), :
        ]


def first_kernel(position_ref, scale_ref, window_ref, high_ref, low_ref, out_ref, v, s, *pairs):
    size, _, block = window_ref.shape
    gram = (high_ref, low_ref)
    load_gram(window_ref, scale_ref[0], high_ref, low_ref)
    begin(window_ref, scale_ref[0], position_ref[0], v, pairs[:3])
    next_gram_steps(gram, v, s, pairs[:3], pairs[3:])
    put_window(v, position_ref[0], out_ref, size, block)


def second_kernel(position_ref, window_ref, high0, low0, out_ref, high1, low1, v, s, kept, *pairs):
    size, _, block = window_ref.shape
    total = v.shape[0]
    gram0, gram1 = (high0, low0), (high1, low1)
    pair, other = pairs[:3], pairs[3:]
    position = position_ref[0]
    load_gram(window_ref, None, high1, low1)
    begin(window_ref, None, position, v, pair)
    next_gram_steps(gram1, v, s, pair, other)

    def keep(rows, value):
        kept[rows, :] = v[rows, :]
        v[rows, :] = value
        thin_store(other, (rows, slice(None)), value)

    product(gram1, pair, keep)
    poly_step(gram1, v, s, other, pair)
    poly_step(gram1, v, s, other, pair)
    step = min(512, total)

    def weights(i, carry):
        rows = pl.ds(pl.multiple_of(i * step, step), step)
        row = lax.broadcasted_iota(jnp.int32, (step, block), 0) + i * step
        col = lax.broadcasted_iota(jnp.int32, (step, block), 1) + position * block
        value = (
            jnp.where(row == col, A_COEF, 0.0) + B_COEF * kept[rows, :] + C_COEF * v[rows, :]
        )
        v[rows, :] = value
        thin_store(pair, (rows, slice(None)), value)
        return carry

    lax.fori_loop(0, total // step, weights, 0)
    poly_step(gram1, v, s, pair, other)
    poly_step(gram0, v, s, pair, other)
    put_window(v, position, out_ref, size, block)


def last_kernel(gain_ref, window_ref, xh_ref, xl_ref, out_ref, high_ref, low_ref):
    load_gram(window_ref, None, high_ref, low_ref)

    def emit(rows, value):
        out_ref[rows, :] = value * gain_ref[0]

    product((high_ref, low_ref), (xh_ref, xl_ref), emit, 256)


def run(kernel, outs, scratch, scalars, arrays):
    return pl.pallas_call(
        kernel,
        out_shape=outs,
        in_specs=[pl.BlockSpec(memory_space=pltpu.SMEM)] * len(scalars)
        + [pl.BlockSpec(memory_space=pltpu.VMEM)] * len(arrays),
        out_specs=jax.tree.map(lambda _: pl.BlockSpec(memory_space=pltpu.VMEM), outs),
        scratch_shapes=scratch,
        compiler_params=pltpu.CompilerParams(vmem_limit_bytes=67043328),
    )(*[jnp.reshape(v, (1,)) for v in scalars], *arrays)


def chain_kernels(window, position, scale_sq, share):
    size, _, block = window.shape
    total = size * block
    full = (total, total)
    thin = (total, block)
    bf16, f32 = jnp.bfloat16, jnp.float32
    half_pairs = [pltpu.VMEM(thin, bf16)] * 6
    slab = jax.ShapeDtypeStruct(window.shape[1:], f32)
    whole = jax.ShapeDtypeStruct(full, bf16)
    high0, low0, mine = run(
        first_kernel,
        (whole, whole, slab),
        [pltpu.VMEM(thin, f32)] * 2 + half_pairs,
        (position, scale_sq),
        (window,),
    )
    window = share(mine)
    mine = run(
        second_kernel,
        slab,
        [pltpu.VMEM(full, bf16)] * 2 + [pltpu.VMEM(thin, f32)] * 3 + half_pairs,
        (position,),
        (window, high0, low0),
    )
    return share(mine)


def apply_kernel(window, x, gain):
    total, wide = x.shape
    xh, xl = halves(x)
    return run(
        last_kernel,
        jax.ShapeDtypeStruct((total, wide), jnp.float32),
        [pltpu.VMEM((total, total), jnp.bfloat16)] * 2,
        (gain,),
        (window, xh, xl),
    )


def chain_plain(window, position, scale_sq, share):
    size, tall, block = window.shape
    total = size * block

    def product_of(gram, v):
        return deep(gram, v, (1, 0))

    def poly(gram, v):
        once = product_of(gram, v)
        return A_COEF * v + B_COEF * once + C_COEF * product_of(gram, once)

    def columns(full):
        return lax.dynamic_slice(full, (0, position * block), (total, block))

    def crop(v):
        return lax.dynamic_slice(
            jnp.concatenate([v, v], axis=0), (position * block, 0), (tall, block)
        )

    gram0 = unfold(window) * scale_sq
    gram1 = unfold(share(crop(poly(gram0, poly(gram0, columns(gram0))))))
    v2 = poly(gram1, poly(gram1, columns(gram1)))
    square = poly(gram1, poly(gram1, product_of(gram1, v2)))
    w = A_COEF * columns(jnp.eye(total, dtype=jnp.float32)) + B_COEF * v2 + C_COEF * square
    return share(crop(poly(gram0, poly(gram1, w))))


def apply_plain(window, x, gain):
    return deep(unfold(window), x, (1, 0)) * gain


def solution(mesh):
    n_fs, n_tp = mesh.shape["fs"], mesh.shape["tp"]
    per = n_fs // GROUPS
    size = per * n_tp
    grid = Mesh(mesh.devices.reshape(GROUPS, per, n_tp), ("g", "h", "tp"))
    fs = ("g", "h")
    team = ("h", "tp")

    def exchange(select, shape, pairs_ok, place):
        me = lax.axis_index(fs)
        held = jnp.zeros((n_fs,) + shape, jnp.float32)
        for shift in range(n_fs):
            dest = (me + shift) % n_fs
            value = select(dest)
            if shift:
                pairs = [(f, (f + shift) % n_fs) for f in range(n_fs)]
                pairs = [p for p in pairs if pairs_ok(*p)]
                value = lax.ppermute(value, fs, pairs)
            source = (me - shift + n_fs) % n_fs
            held = lax.dynamic_update_slice(held, value[None], (source, 0, 0))
        return held

    def local(weights_in, weights_mix, momentum_in, momentum_mix, grads_in, grads_mix):
        moment_in = MOMENTUM_DECAY * momentum_in + grads_in
        moment_mix = MOMENTUM_DECAY * momentum_mix + grads_mix
        rows, cols_in = moment_in.shape[1:]
        cols_mix = moment_mix.shape[1]
        wide, narrow = cols_in // per, cols_mix // per
        total = rows * n_fs
        block = total // size
        window = (size // 2 + 1) * block
        group = lax.axis_index("g")
        member = lax.axis_index(team)

        def pick_in(dest):
            which = jnp.clip(dest // per - IN_GROUPS[0], 0, 1)
            return lax.dynamic_slice(moment_in, (which, 0, (dest % per) * wide), (1, rows, wide))[0]

        def pick_mix(dest):
            return lax.dynamic_slice(moment_mix, (0, (dest % per) * narrow), (rows, narrow))

        got_in = exchange(pick_in, (rows, wide), lambda f, d: d // per in IN_GROUPS, None)
        got_mix = exchange(pick_mix, (rows, narrow), lambda f, d: d // per == MIX_GROUP, None)
        x = jnp.where(
            group == MIX_GROUP, jnp.pad(got_mix, ((0, 0), (0, 0), (0, wide - narrow))), got_in
        ).reshape(total, wide)

        def share(mine):
            return lax.all_gather(mine, team, axis=0, tiled=False)

        twice = jnp.concatenate([x, x[: window - block]], axis=0)
        partial = jnp.stack(
            [
                lax.dot_general(
                    twice[i * block : i * block + window],
                    x[i * block : (i + 1) * block],
                    (((1,), (1,)), ((), ())),
                    precision=lax.Precision.HIGHEST,
                )
                for i in range(size)
            ]
        )
        gram_window = share(lax.psum_scatter(partial, team, scatter_dimension=0, tiled=False))
        corner = jnp.eye(block, dtype=jnp.float32)
        ssq = jnp.sum(gram_window[:, :block, :] * corner)
        scaling = 0.5 * lax.rsqrt(jnp.maximum(ssq / total, 1.0))
        columns = jnp.where(group == MIX_GROUP, cols_mix, cols_in) * n_tp
        gain = jnp.sqrt(jnp.maximum(columns, total).astype(jnp.float32)) * scaling
        kernels = block % 128 == 0
        chain = chain_kernels if kernels else chain_plain
        apply = apply_kernel if kernels else apply_plain
        w_window = chain(gram_window, member, scaling**2, share)
        update = apply(w_window, x, gain).reshape(n_fs, rows, wide)

        def out_in(dest):
            return lax.dynamic_slice(update, (dest, 0, 0), (1, rows, wide))[0]

        def out_mix(dest):
            return lax.dynamic_slice(update, (dest, 0, 0), (1, rows, narrow))[0]

        back_in = exchange(out_in, (rows, wide), lambda f, d: f // per in IN_GROUPS, None)
        back_mix = exchange(out_mix, (rows, narrow), lambda f, d: f // per == MIX_GROUP, None)
        step_in = jnp.stack(
            [
                jnp.concatenate([back_in[g * per + h] for h in range(per)], axis=1)
                for g in IN_GROUPS
            ]
        )
        step_mix = jnp.concatenate(
            [back_mix[MIX_GROUP * per + h] for h in range(per)], axis=1
        )
        return (
            moment_in,
            moment_mix,
            weights_in - STEP_RATE * step_in,
            weights_mix - STEP_RATE * step_mix,
            step_in,
            step_mix,
        )

    big = P(None, fs, "tp")
    small = P(fs, "tp")
    specs = (big, small, big, small, big, small)
    return jax.shard_map(local, mesh=grid, in_specs=specs, out_specs=specs, check_vma=False)
```
